32 devices in a mesh: grp: 2 (over y), ep: 4 (over z), tp: 4 (over x, core).
Axes of the slice: x: 2, y: 2, z: 4, core: 2. Of those that a mesh axis runs over, the one named last changes fastest.
Arguments:
- mixer_tokens: bfloat16 [4096, 2048], P(('grp', 'ep', 'tp')), parts along dimension 0, may hold values from -6 to 6
- mixer_gain: bfloat16 [2048], replicated, may hold values from 0.099609375 to 1.8984375
- in_weight: bfloat16 [2048, 2048], P(None, 'tp'), may hold values from -0.125 to 0.125
- group_weight: bfloat16 [4, 512, 512], P('tp'), may hold values from -0.25 to 0.25
- channel_scale: bfloat16 [2048], P('tp'), may hold values from 0.099609375 to 1.8984375
- out_weight: bfloat16 [2048, 2048], P('tp'), may hold values from -0.125 to 0.125
- expert_tokens: bfloat16 [4096, 2048], P(('grp', 'ep', 'tp')), parts along dimension 0, may hold values from -6 to 6
- expert_gain: bfloat16 [2048], replicated, may hold values from 0.099609375 to 1.8984375
- route_ids: int32 [4096, 2], P(('grp', 'ep', 'tp')), parts along dimension 0, may hold values from 0 to 3, all different within a row; in each aligned block of 128 rows (0 to 127, 128 to 255, ...) at most 128 rows name the same one
- route_weights: float32 [4096, 2], P(('grp', 'ep', 'tp')), parts along dimension 0, may hold values from 0.1 to 1
- gate_weight: bfloat16 [4, 2048, 1024], P('ep', None, 'tp'), may hold values from -0.125 to 0.125
- up_weight: bfloat16 [4, 2048, 1024], P('ep', None, 'tp'), may hold values from -0.125 to 0.125
- down_weight: bfloat16 [4, 1024, 2048], P('ep', 'tp'), may hold values from -0.1875 to 0.1875
Outputs:
- mixed_tokens: bfloat16 [4096, 2048], P(('grp', 'ep', 'tp')), parts along dimension 0
- expert_mix: bfloat16 [4096, 2048], P(('grp', 'ep', 'tp')), parts along dimension 0
The draws below stay inside these ranges and needn't reach their ends.
There are 2 independent parts, one for each index of `grp`. The reference program is written for one: setup_inputs(seed, part) draws one part's arguments, and reference() takes and returns one part's arrays. A program takes and returns all parts, laid end to end along the dimension named above; an argument that names none is the same for every part. Nothing has to cross between parts.
Inputs may be any that keep to these rules, and one draw needn't show every extreme that they name: `route_ids`: each row names 2 different experts; in the rows of one device no expert is named more than 128 times, and one expert exactly 128 times in the rows of some device.
All inputs are finite; a program needn't handle non-finite values.
Results may differ from the reference program's by a relative error of at most 0.015.
Values may be sent and summed in bfloat16 or wider, within the bound.
A program may use at most 128 MiB of HBM per device.

```python
import math
import jax
import jax.numpy as jnp
import numpy as np
from jax import lax

D = 2048
GROUPS = 4
GW = 512
FF = 1024
FF_DEV = 256
TOP = 2
TOK_DEV = 128
TOKENS = 2048
EXPERTS = 4
CAP = 128
N_EP = 4
N_TP = 4


def block_levels(key, dims, split, least, high):
    def one(position, shards_of):
        heights = jax.random.uniform(jax.random.fold_in(jax.random.fold_in(key, 6), position), (shards_of,), jnp.float32, least / len(split), high / len(split))
        return jnp.repeat(jnp.exp(heights), dims[position] // shards_of).reshape((-1,) + (1,) * (len(dims) - position - 1))

    level = one(*split[0])
    for cut in split[1:]:
        level = level * one(*cut)
    return level


def routed_block(own_key, own, number, rows, number_of, top, bound, lean):
    order = jax.random.permutation(own_key, number_of)
    heavy_load, ordinary = portions_of(number_of, rows * top, bound, lean, True), portions_of(number_of, rows * top, bound, lean, False)
    places = jnp.arange(number_of)

    def named(lengths, rotation):
        used = int((lengths > 0).sum())
        fixed = max(1, used // 4)
        moved = fixed + (places - fixed + rotation * (used - fixed)) % max(1, number_of - fixed)
        return jnp.zeros((number_of,), jnp.int32).at[order[jnp.where(places < fixed, places, moved)]].set(jnp.asarray(lengths, jnp.int32))

    lengths = jnp.where(number % 4 == 0, named(heavy_load, number // 4), named(ordinary, number - number // 4 - 1))
    mixed = jax.random.permutation(jax.random.fold_in(own, 3), number_of)
    source_of, taker = mixed[0:number_of // 2 * 2:2], mixed[1:number_of // 2 * 2:2]
    room = jnp.minimum(lengths[source_of] - 1, bound - lengths[taker]) // 2
    room = jnp.where((source_of == order[0]) | (taker == order[0]) | (lengths[taker] == 0), 0, jnp.maximum(room, 0))
    moved = jax.random.randint(jax.random.fold_in(own, 4), (number_of // 2,), 0, 1 << 20) % (room + 1)
    lengths = lengths.at[source_of].add(-moved).at[taker].add(moved)
    labels = jnp.searchsorted(jnp.cumsum(lengths), jnp.arange(rows * top), side="right").astype(jnp.int32)
    listing = labels.reshape(top, rows).T
    listing = listing[jax.random.permutation(jax.random.fold_in(own, 1), rows)]
    rotation = jax.random.randint(jax.random.fold_in(own, 2), (rows, 1), 0, top)
    return jnp.take_along_axis(listing, (jnp.arange(top)[None, :] + rotation) % top, axis=1)


def portions_of(number_of, total, most, lean, full):
    loads = [(1 << 20) // math.isqrt(rank ** lean) + 1 for rank in range(1, number_of + 1)]
    largest = most if full else min(most, max(-(-total // number_of), total * loads[0] // sum(loads)))
    least = 1 if total - largest >= number_of - 1 else 0
    holding, spare = [largest] + [least] * (number_of - 1), total - largest - least * (number_of - 1)
    while spare > 0:
        free = [i for i in range(1, number_of) if holding[i] < largest] or [i for i in range(1, number_of) if holding[i] < most]
        pool, budget = sum([loads[i] for i in free]), spare
        for i in free:
            more = min(most - holding[i], max(1, budget * loads[i] // pool), spare)
            holding[i] = holding[i] + more
            spare = spare - more
    return np.array(holding)


def bell_draw(key, shape, scale, bound, split=(), kind=jnp.bfloat16):
    entries = jax.random.normal(key, shape, jnp.float32) * scale
    if len(split) > 0:
        entries = block_levels(key, shape, split, -0.22, 0.18) * entries
    return jnp.clip(entries, min=-bound, max=bound).astype(kind)


def setup_inputs(seed: int = 0, part: int = 0) -> dict:
    splits = jax.random.split(jax.random.key(seed), 14)
    part_keys = jax.random.split(jax.random.fold_in(splits[13], part), 14)
    mixer_tokens = bell_draw(part_keys[0], (TOKENS, D), 1.0, 6.0, ((0, 16),))
    mixer_gain = jnp.clip(1.0 + 0.18 * jax.random.normal(splits[1], (D,), jnp.float32), 0.099609375, 1.8984375).astype(jnp.bfloat16)
    in_weight = bell_draw(splits[2], (D, D), D ** -0.5, 0.125, ((1, 4),))
    group_weight = bell_draw(splits[3], (GROUPS, GW, GW), GW ** -0.5, 0.25, ((0, 4),))
    channel_scale = jnp.clip(1.0 + 0.18 * jax.random.normal(splits[4], (D,), jnp.float32), 0.099609375, 1.8984375).astype(jnp.bfloat16)
    out_weight = bell_draw(splits[5], (D, D), D ** -0.5, 0.125, ((0, 4),))
    expert_tokens = bell_draw(part_keys[6], (TOKENS, D), 1.0, 6.0, ((0, 16),))
    expert_gain = jnp.clip(1.0 + 0.18 * jax.random.normal(splits[7], (D,), jnp.float32), 0.099609375, 1.8984375).astype(jnp.bfloat16)
    route_ids_keys = jax.random.split(jax.random.fold_in(part_keys[8], 1), TOKENS // TOK_DEV)
    route_ids_turns = jax.random.permutation(jax.random.fold_in(part_keys[8], 3), TOKENS // TOK_DEV)
    route_ids = jax.vmap(lambda own, number: routed_block(jax.random.fold_in(part_keys[8], 2), own, number, TOK_DEV, EXPERTS, TOP, CAP, 2))(route_ids_keys, route_ids_turns).reshape((TOKENS, TOP))
    route_weights = jnp.clip(jnp.exp(math.log(1.0) - 2.3025851 * jax.random.uniform(part_keys[9], (TOKENS, TOP), jnp.float32) ** block_levels(part_keys[9], (TOKENS, TOP), ((0, 16),), -0.2, 0.2)), 0.1, 1.0)
    gate_weight = bell_draw(splits[10], (EXPERTS, D, FF), D ** -0.5, 0.125, ((0, 4), (2, 4)))
    up_weight = bell_draw(splits[11], (EXPERTS, D, FF), D ** -0.5, 0.125, ((0, 4), (2, 4)))
    down_weight = bell_draw(splits[12], (EXPERTS, FF, D), FF ** -0.5, 0.1875, ((0, 4), (1, 4)))
    return dict(mixer_tokens=mixer_tokens, mixer_gain=mixer_gain, in_weight=in_weight, group_weight=group_weight, channel_scale=channel_scale, out_weight=out_weight, expert_tokens=expert_tokens, expert_gain=expert_gain, route_ids=route_ids, route_weights=route_weights, gate_weight=gate_weight, up_weight=up_weight, down_weight=down_weight)


def rms_rows(rows, gain):
    values = rows.astype(jnp.float32)
    scaled = values * lax.rsqrt(lax.optimization_barrier(jnp.mean(values * values, axis=-1, keepdims=True)) + 1e-06)
    return (scaled * gain.astype(jnp.float32)).astype(jnp.bfloat16)

def expert_hidden(rows, w_gate, w_up):
    gate = jnp.dot(rows, w_gate, preferred_element_type=jnp.float32)
    upper = jnp.dot(rows, w_up, preferred_element_type=jnp.float32)
    return (jax.nn.silu(gate) * upper).astype(jnp.bfloat16)

def reference(mixer_tokens, mixer_gain, in_weight, group_weight, channel_scale, out_weight, expert_tokens, expert_gain, route_ids, route_weights, gate_weight, up_weight, down_weight):
    normed = rms_rows(mixer_tokens, mixer_gain)
    pooled_in = jnp.dot(normed, in_weight, preferred_element_type=jnp.float32).astype(jnp.bfloat16)
    values = pooled_in.astype(jnp.float32)
    length = values.shape[0]
    prefix = jnp.concatenate([jnp.zeros((1, D), jnp.float32), jnp.cumsum(values, axis=0)], axis=0)
    mixed = jnp.zeros((length, D), jnp.float32)
    for group in range(GROUPS):
        window = 2 ** (group + 1)
        low_col = group * GW
        upper = prefix[1:, low_col:low_col + GW]
        lower = jnp.concatenate([jnp.zeros((window - 1, GW), jnp.float32), prefix[:length - window + 1, low_col:low_col + GW]], axis=0)
        counts = jnp.minimum(jnp.arange(1, length + 1), window).astype(jnp.float32)
        trail = ((upper - lower) / counts[:, None] - values[:, low_col:low_col + GW]).astype(jnp.bfloat16)
        grouped = (jnp.dot(trail, group_weight[group], preferred_element_type=jnp.float32) * channel_scale[low_col:low_col + GW].astype(jnp.float32)).astype(jnp.bfloat16)
        partial_value = jnp.dot(grouped, out_weight[low_col:low_col + GW, :], preferred_element_type=jnp.float32)
        partial_value = lax.optimization_barrier(partial_value.astype(jnp.bfloat16))
        mixed = mixed + partial_value.astype(jnp.float32)
    mixed_tokens = mixed.astype(jnp.bfloat16)
    expert_in = rms_rows(expert_tokens, expert_gain)
    weights = route_weights.astype(jnp.float32)
    shares = weights / lax.optimization_barrier(jnp.sum(weights, axis=1, keepdims=True))
    count_tok = expert_in.shape[0]
    flat_ids = route_ids.reshape(count_tok * TOP).astype(jnp.int32)
    flat_tokens = jnp.concatenate([(jnp.arange(count_tok * TOP) // TOP).astype(jnp.int32), jnp.full((1,), count_tok, jnp.int32)])
    flat_shares = jnp.concatenate([shares.reshape(count_tok * TOP), jnp.zeros((1,), jnp.float32)])
    padded = jnp.concatenate([expert_in, jnp.zeros((1, D), jnp.bfloat16)], axis=0)
    most = N_EP * N_TP * CAP

    def one_expert(total, expert):
        chosen = jnp.nonzero(flat_ids == expert, size=most, fill_value=count_tok * TOP)[0].astype(jnp.int32)
        token_of = flat_tokens[chosen]
        rows = padded[token_of]
        hidden = expert_hidden(rows, gate_weight[expert], up_weight[expert])
        result = jnp.zeros((most, D), jnp.float32)
        for block in range(N_TP):
            part = jnp.dot(hidden[:, block * FF_DEV:(block + 1) * FF_DEV], down_weight[expert][block * FF_DEV:(block + 1) * FF_DEV, :], preferred_element_type=jnp.float32)
            part = lax.optimization_barrier(part.astype(jnp.bfloat16))
            result = result + part.astype(jnp.float32)
        total = total.at[token_of].add(result * flat_shares[chosen][:, None])
        return (total, None)
    total, _ = lax.scan(one_expert, jnp.zeros((count_tok + 1, D), jnp.float32), jnp.arange(EXPERTS).astype(jnp.int32))
    expert_mix = total[:count_tok].astype(jnp.bfloat16)
    return (mixed_tokens, expert_mix)
```

```python
import jax
import jax.numpy as jnp
from jax import lax
from jax.sharding import PartitionSpec as P

WINDOW_MAX = 16


def shifted(value, axis, by):
    devices = lax.axis_size(axis)
    pairs = [(i, i + by) for i in range(devices) if 0 <= i + by < devices]
    return lax.ppermute(value, axis, pairs)


def rms_rows(rows, gain):
    values = rows.astype(jnp.float32)
    scaled = values * lax.rsqrt(jnp.mean(values * values, axis=-1, keepdims=True) + 1e-06)
    return (scaled * gain.astype(jnp.float32)).astype(jnp.bfloat16)


def expert_hidden(rows, w_gate, w_up):
    gate = jnp.dot(rows, w_gate, preferred_element_type=jnp.float32)
    upper = jnp.dot(rows, w_up, preferred_element_type=jnp.float32)
    return (jax.nn.silu(gate) * upper).astype(jnp.bfloat16)


def local(
    mixer_tokens,
    mixer_gain,
    in_weight,
    group_weight,
    channel_scale,
    out_weight,
    expert_tokens,
    expert_gain,
    route_ids,
    route_weights,
    gate_weight,
    up_weight,
    down_weight,
):
    normed = rms_rows(mixer_tokens, mixer_gain)
    pooled_in = jnp.dot(
        lax.all_gather(normed, "tp", axis=0, tiled=True),
        in_weight,
        preferred_element_type=jnp.float32,
    ).astype(jnp.bfloat16)
    block_rows = pooled_in.shape[0]
    rim_rows = shifted(pooled_in[block_rows - WINDOW_MAX :], "ep", 1)
    values = pooled_in.astype(jnp.float32)
    extended = jnp.concatenate([rim_rows.astype(jnp.float32), values], axis=0)
    window = jnp.left_shift(jnp.int32(2), lax.axis_index("tp"))
    sums = extended
    span = 1
    total = jnp.zeros_like(values)
    for level in range(WINDOW_MAX.bit_length() - 1):
        sums = sums[span:] + sums[:-span]
        span = span * 2
        total = total + jnp.where(window == span, sums[sums.shape[0] - block_rows :], 0.0)
    positions = lax.axis_index("ep") * block_rows + lax.iota(jnp.int32, block_rows) + 1
    counts = jnp.minimum(positions, window).astype(jnp.float32)
    pooled = (total / counts[:, None] - values).astype(jnp.bfloat16)
    grouped = (
        jnp.dot(pooled, group_weight[0], preferred_element_type=jnp.float32)
        * channel_scale.astype(jnp.float32)
    ).astype(jnp.bfloat16)
    rows = grouped
    mixed_tokens = lax.psum_scatter(
        jnp.dot(rows, out_weight, preferred_element_type=jnp.float32).astype(jnp.bfloat16),
        "tp",
        scatter_dimension=0,
        tiled=True,
    )
    expert_in = rms_rows(expert_tokens, expert_gain)
    shares = route_weights / jnp.sum(route_weights, axis=1, keepdims=True)
    rows_here, top_k = route_ids.shape
    width = expert_in.shape[1]
    n_experts = lax.axis_size("ep") * gate_weight.shape[0]
    capacity = 4 * rows_here // n_experts
    if capacity >= rows_here:
        experts = jnp.arange(n_experts, dtype=jnp.int32)
        named = (route_ids[:, :, None] == experts[None, None, :]).astype(jnp.float32)
        coefs = jnp.sum(named * shares[:, :, None], axis=1)
        every = lax.all_gather(expert_in, ("ep", "tp"), axis=0, tiled=True)
        coefs = lax.all_gather(coefs, ("ep", "tp"), axis=0, tiled=True)
        mine = (experts == lax.axis_index("ep")).astype(jnp.float32)
        coef = jnp.sum(coefs * mine[None, :], axis=1, keepdims=True)
        hidden = expert_hidden(every, gate_weight[0], up_weight[0])
        part = jnp.dot(hidden, down_weight[0], preferred_element_type=jnp.float32) * coef
        expert_mix = lax.psum_scatter(
            part.astype(jnp.bfloat16), ("ep", "tp"), scatter_dimension=0, tiled=True
        )
        return (mixed_tokens, expert_mix)
    flat_ids = route_ids.reshape(rows_here * top_k)
    one_hot = (flat_ids[:, None] == jnp.arange(n_experts, dtype=jnp.int32)[None, :]).astype(
        jnp.int32
    )
    before = jnp.cumsum(one_hot, axis=0) - one_hot
    slots = jnp.sum(before * one_hot, axis=1)
    targets = flat_ids * capacity + slots
    placement = (
        targets.reshape(rows_here, top_k)[None, :, :]
        == jnp.arange(n_experts * capacity, dtype=jnp.int32)[:, None, None]
    )
    dispatch = jnp.any(placement, axis=2).astype(jnp.bfloat16)
    outgoing = jnp.dot(dispatch, expert_in, preferred_element_type=jnp.float32).astype(jnp.bfloat16)
    outgoing = outgoing.reshape(n_experts, capacity, width)
    arrived = lax.all_to_all(outgoing, "ep", split_axis=0, concat_axis=0, tiled=True)
    sources, held, _ = arrived.shape
    flat = arrived.reshape(sources * held, width)
    hidden = expert_hidden(
        lax.all_gather(flat, "tp", axis=0, tiled=True), gate_weight[0], up_weight[0]
    )
    rows = hidden
    summed = lax.psum_scatter(
        jnp.dot(rows, down_weight[0], preferred_element_type=jnp.float32).astype(jnp.bfloat16),
        "tp",
        scatter_dimension=0,
        tiled=True,
    ).astype(jnp.float32)
    expert_out = lax.all_to_all(
        summed.reshape(sources, held, width).astype(jnp.bfloat16),
        "ep",
        split_axis=0,
        concat_axis=0,
        tiled=True,
    ).astype(jnp.float32)
    flat_out = expert_out.reshape(n_experts * capacity, width)
    picked = jnp.take(flat_out, targets, axis=0).reshape(rows_here, top_k, width)
    expert_mix = jnp.sum(picked * shares[:, :, None], axis=1).astype(jnp.bfloat16)
    return (mixed_tokens, expert_mix)


def solution(mesh):
    placed = (
        P(("grp", "ep", "tp"), None),
        P(),
        P(None, "tp"),
        P("tp", None, None),
        P("tp"),
        P("tp", None),
        P(("grp", "ep", "tp"), None),
        P(),
        P(("grp", "ep", "tp"), None),
        P(("grp", "ep", "tp"), None),
        P("ep", None, "tp"),
        P("ep", None, "tp"),
        P("ep", "tp", None),
    )
    return jax.shard_map(
        local,
        mesh=mesh,
        in_specs=placed,
        out_specs=(P(("grp", "ep", "tp"), None), P(("grp", "ep", "tp"), None)),
        check_vma=False,
    )
```

```python
import jax
import jax.numpy as jnp
from jax import lax
from jax.sharding import PartitionSpec as P

WINDOW_MAX = 16


def shifted(value, axis, by):
    devices = lax.axis_size(axis)
    pairs = [(i, i + by) for i in range(devices) if 0 <= i + by < devices]
    return lax.ppermute(value, axis, pairs)


def turned(value, axis, by):
    devices = lax.axis_size(axis)
    if by % devices == 0:
        return value
    return lax.ppermute(value, axis, [(i, (i + by) % devices) for i in range(devices)])


def rms_rows(rows, gain):
    values = rows.astype(jnp.float32)
    scaled = values * lax.rsqrt(jnp.mean(values * values, axis=-1, keepdims=True) + 1e-06)
    return (scaled * gain.astype(jnp.float32)).astype(jnp.bfloat16)


def expert_hidden(rows, w_gate, w_up):
    gate = jnp.dot(rows, w_gate, preferred_element_type=jnp.float32)
    upper = jnp.dot(rows, w_up, preferred_element_type=jnp.float32)
    return (jax.nn.silu(gate) * upper).astype(jnp.bfloat16)


def local(
    mixer_tokens,
    mixer_gain,
    in_weight,
    group_weight,
    channel_scale,
    out_weight,
    expert_tokens,
    expert_gain,
    route_ids,
    route_weights,
    gate_weight,
    up_weight,
    down_weight,
):
    normed = rms_rows(mixer_tokens, mixer_gain)
    expert_in = rms_rows(expert_tokens, expert_gain)
    shares = route_weights / jnp.sum(route_weights, axis=1, keepdims=True)
    rows_here, top_k = route_ids.shape
    width = expert_in.shape[1]
    n_experts = lax.axis_size("ep") * gate_weight.shape[0]
    capacity = 4 * rows_here // n_experts
    dense = capacity >= rows_here
    parts_tp = lax.axis_size("tp")
    if dense:
        both = lax.all_gather(jnp.concatenate([normed, expert_in], axis=0), "tp", axis=0, tiled=True)
        both = both.reshape(parts_tp, 2, rows_here, width)
        every = both[:, 0].reshape(parts_tp * rows_here, width)
        own = both[:, 1].reshape(parts_tp * rows_here, width)
    else:
        every = lax.all_gather(normed, "tp", axis=0, tiled=True)
    pooled_in = jnp.dot(
        every,
        in_weight,
        preferred_element_type=jnp.float32,
    ).astype(jnp.bfloat16)
    block_rows = pooled_in.shape[0]
    rim_rows = shifted(pooled_in[block_rows - WINDOW_MAX :], "ep", 1)
    values = pooled_in.astype(jnp.float32)
    extended = jnp.concatenate([rim_rows.astype(jnp.float32), values], axis=0)
    window = jnp.left_shift(jnp.int32(2), lax.axis_index("tp"))
    sums = extended
    span = 1
    total = jnp.zeros_like(values)
    for level in range(WINDOW_MAX.bit_length() - 1):
        sums = sums[span:] + sums[:-span]
        span = span * 2
        total = total + jnp.where(window == span, sums[sums.shape[0] - block_rows :], 0.0)
    positions = lax.axis_index("ep") * block_rows + lax.iota(jnp.int32, block_rows) + 1
    counts = jnp.minimum(positions, window).astype(jnp.float32)
    pooled = (total / counts[:, None] - values).astype(jnp.bfloat16)
    grouped = (
        jnp.dot(pooled, group_weight[0], preferred_element_type=jnp.float32)
        * channel_scale.astype(jnp.float32)
    ).astype(jnp.bfloat16)
    mixed_part = jnp.dot(grouped, out_weight, preferred_element_type=jnp.float32).astype(
        jnp.bfloat16
    )
    if dense:
        experts = jnp.arange(n_experts, dtype=jnp.int32)
        named = (route_ids[:, :, None] == experts[None, None, :]).astype(jnp.float32)
        coefs = jnp.sum(named * shares[:, :, None], axis=1)
        coefs = lax.all_gather(coefs, ("ep", "tp"), axis=0, tiled=True)
        blocks = lax.axis_size("ep")
        here = lax.axis_index("ep")
        mine = (experts == here).astype(jnp.float32)
        coef = jnp.sum(coefs * mine[None, :], axis=1).reshape(blocks, parts_tp, rows_here)
        order = list(range(1, blocks))

        def scale_of(k):
            return lax.dynamic_index_in_dim(coef, lax.rem(here - k + blocks, blocks), 0, False)

        def expert_part(rows, scale):
            hidden = expert_hidden(rows, gate_weight[0], up_weight[0])
            part = jnp.dot(hidden, down_weight[0], preferred_element_type=jnp.float32)
            return (part * scale.reshape(-1)[:, None]).astype(jnp.bfloat16)

        moved = jnp.concatenate([turned(expert_in, "ep", k) for k in order], axis=0)
        moved, own = lax.optimization_barrier((moved, own))
        own_part = expert_part(own, scale_of(0))
        others = lax.all_gather(moved, "tp", axis=0, tiled=True)
        part = expert_part(others, jnp.stack([scale_of(k) for k in order], axis=1))
        back = lax.psum_scatter(part, "tp", scatter_dimension=0, tiled=True)
        back = back.reshape(blocks - 1, rows_here, width)
        pair = jnp.stack(
            [value.reshape(parts_tp, rows_here, width) for value in (mixed_part, own_part)], axis=1
        ).reshape(2 * parts_tp * rows_here, width)
        pair = lax.psum_scatter(pair, "tp", scatter_dimension=0, tiled=True)
        total = pair[rows_here:].astype(jnp.float32)
        for i, k in enumerate(order):
            total = total + turned(back[i], "ep", -k).astype(jnp.float32)
        return (pair[:rows_here], total.astype(jnp.bfloat16))
    mixed_tokens = lax.psum_scatter(mixed_part, "tp", scatter_dimension=0, tiled=True)
    flat_ids = route_ids.reshape(rows_here * top_k)
    one_hot = (flat_ids[:, None] == jnp.arange(n_experts, dtype=jnp.int32)[None, :]).astype(
        jnp.int32
    )
    before = jnp.cumsum(one_hot, axis=0) - one_hot
    slots = jnp.sum(before * one_hot, axis=1)
    targets = flat_ids * capacity + slots
    placement = (
        targets.reshape(rows_here, top_k)[None, :, :]
        == jnp.arange(n_experts * capacity, dtype=jnp.int32)[:, None, None]
    )
    dispatch = jnp.any(placement, axis=2).astype(jnp.bfloat16)
    outgoing = jnp.dot(dispatch, expert_in, preferred_element_type=jnp.float32).astype(jnp.bfloat16)
    outgoing = outgoing.reshape(n_experts, capacity, width)
    arrived = lax.all_to_all(outgoing, "ep", split_axis=0, concat_axis=0, tiled=True)
    sources, held, _ = arrived.shape
    flat = arrived.reshape(sources * held, width)
    hidden = expert_hidden(
        lax.all_gather(flat, "tp", axis=0, tiled=True), gate_weight[0], up_weight[0]
    )
    rows = hidden
    summed = lax.psum_scatter(
        jnp.dot(rows, down_weight[0], preferred_element_type=jnp.float32).astype(jnp.bfloat16),
        "tp",
        scatter_dimension=0,
        tiled=True,
    ).astype(jnp.float32)
    expert_out = lax.all_to_all(
        summed.reshape(sources, held, width).astype(jnp.bfloat16),
        "ep",
        split_axis=0,
        concat_axis=0,
        tiled=True,
    ).astype(jnp.float32)
    flat_out = expert_out.reshape(n_experts * capacity, width)
    picked = jnp.take(flat_out, targets, axis=0).reshape(rows_here, top_k, width)
    expert_mix = jnp.sum(picked * shares[:, :, None], axis=1).astype(jnp.bfloat16)
    return (mixed_tokens, expert_mix)


def solution(mesh):
    placed = (
        P(("grp", "ep", "tp"), None),
        P(),
        P(None, "tp"),
        P("tp", None, None),
        P("tp"),
        P("tp", None),
        P(("grp", "ep", "tp"), None),
        P(),
        P(("grp", "ep", "tp"), None),
        P(("grp", "ep", "tp"), None),
        P("ep", None, "tp"),
        P("ep", None, "tp"),
        P("ep", "tp", None),
    )
    return jax.shard_map(
        local,
        mesh=mesh,
        in_specs=placed,
        out_specs=(P(("grp", "ep", "tp"), None), P(("grp", "ep", "tp"), None)),
        check_vma=False,
    )
```

```python
import jax
import jax.numpy as jnp
from jax import lax
from jax.sharding import PartitionSpec as P

WINDOW_MAX = 16


def shifted(value, axis, by):
    devices = lax.axis_size(axis)
    pairs = [(i, i + by) for i in range(devices) if 0 <= i + by < devices]
    return lax.ppermute(value, axis, pairs)


def turned(value, axis, by):
    devices = lax.axis_size(axis)
    if by % devices == 0:
        return value
    return lax.ppermute(value, axis, [(i, (i + by) % devices) for i in range(devices)])


def rms_rows(rows, gain):
    values = rows.astype(jnp.float32)
    scaled = values * lax.rsqrt(jnp.mean(values * values, axis=-1, keepdims=True) + 1e-06)
    return (scaled * gain.astype(jnp.float32)).astype(jnp.bfloat16)


def expert_hidden(rows, w_gate, w_up):
    gate = jnp.dot(rows, w_gate, preferred_element_type=jnp.float32)
    upper = jnp.dot(rows, w_up, preferred_element_type=jnp.float32)
    return (jax.nn.silu(gate) * upper).astype(jnp.bfloat16)


def local(
    mixer_tokens,
    mixer_gain,
    in_weight,
    group_weight,
    channel_scale,
    out_weight,
    expert_tokens,
    expert_gain,
    route_ids,
    route_weights,
    gate_weight,
    up_weight,
    down_weight,
):
    normed = rms_rows(mixer_tokens, mixer_gain)
    expert_in = rms_rows(expert_tokens, expert_gain)
    shares = route_weights / jnp.sum(route_weights, axis=1, keepdims=True)
    rows_here, top_k = route_ids.shape
    width = expert_in.shape[1]
    n_experts = lax.axis_size("ep") * gate_weight.shape[0]
    capacity = 4 * rows_here // n_experts
    dense = capacity >= rows_here
    parts_tp = lax.axis_size("tp")
    every = lax.all_gather(normed, "tp", axis=0, tiled=True)
    if dense:
        moved = [turned(expert_in, "ep", k) for k in range(lax.axis_size("ep"))]
        moved, every = lax.optimization_barrier((jnp.concatenate(moved, axis=0), every))
    pooled_in = jnp.dot(
        every,
        in_weight,
        preferred_element_type=jnp.float32,
    ).astype(jnp.bfloat16)
    block_rows = pooled_in.shape[0]
    rim_rows = shifted(pooled_in[block_rows - WINDOW_MAX :], "ep", 1)
    values = pooled_in.astype(jnp.float32)
    extended = jnp.concatenate([rim_rows.astype(jnp.float32), values], axis=0)
    window = jnp.left_shift(jnp.int32(2), lax.axis_index("tp"))
    sums = extended
    span = 1
    total = jnp.zeros_like(values)
    for level in range(WINDOW_MAX.bit_length() - 1):
        sums = sums[span:] + sums[:-span]
        span = span * 2
        total = total + jnp.where(window == span, sums[sums.shape[0] - block_rows :], 0.0)
    positions = lax.axis_index("ep") * block_rows + lax.iota(jnp.int32, block_rows) + 1
    counts = jnp.minimum(positions, window).astype(jnp.float32)
    pooled = (total / counts[:, None] - values).astype(jnp.bfloat16)
    grouped = (
        jnp.dot(pooled, group_weight[0], preferred_element_type=jnp.float32)
        * channel_scale.astype(jnp.float32)
    ).astype(jnp.bfloat16)
    mixed_part = jnp.dot(grouped, out_weight, preferred_element_type=jnp.float32).astype(
        jnp.bfloat16
    )
    if dense:
        experts = jnp.arange(n_experts, dtype=jnp.int32)
        named = (route_ids[:, :, None] == experts[None, None, :]).astype(jnp.float32)
        coefs = jnp.sum(named * shares[:, :, None], axis=1)
        coefs = lax.all_gather(coefs, ("ep", "tp"), axis=0, tiled=True)
        blocks = lax.axis_size("ep")
        here = lax.axis_index("ep")
        mine = (experts == here).astype(jnp.float32)
        coef = jnp.sum(coefs * mine[None, :], axis=1).reshape(blocks, parts_tp, rows_here)
        order = list(range(blocks))

        def scale_of(k):
            return lax.dynamic_index_in_dim(coef, lax.rem(here - k + blocks, blocks), 0, False)

        def expert_part(rows, scale):
            hidden = expert_hidden(rows, gate_weight[0], up_weight[0])
            part = jnp.dot(hidden, down_weight[0], preferred_element_type=jnp.float32)
            return (part * scale.reshape(-1)[:, None]).astype(jnp.bfloat16)

        others = lax.all_gather(moved, "tp", axis=0, tiled=True)
        part = expert_part(others, jnp.stack([scale_of(k) for k in order], axis=1))
        back = lax.psum_scatter(part, "tp", scatter_dimension=0, tiled=True)
        mixed_part, back = lax.optimization_barrier((mixed_part, back))
        back = back.reshape(blocks, rows_here, width)
        total = jnp.zeros((rows_here, width), jnp.float32)
        for i, k in enumerate(order):
            total = total + turned(back[i], "ep", -k).astype(jnp.float32)
        mixed_tokens = lax.psum_scatter(mixed_part, "tp", scatter_dimension=0, tiled=True)
        return (mixed_tokens, total.astype(jnp.bfloat16))
    mixed_tokens = lax.psum_scatter(mixed_part, "tp", scatter_dimension=0, tiled=True)
    flat_ids = route_ids.reshape(rows_here * top_k)
    one_hot = (flat_ids[:, None] == jnp.arange(n_experts, dtype=jnp.int32)[None, :]).astype(
        jnp.int32
    )
    before = jnp.cumsum(one_hot, axis=0) - one_hot
    slots = jnp.sum(before * one_hot, axis=1)
    targets = flat_ids * capacity + slots
    placement = (
        targets.reshape(rows_here, top_k)[None, :, :]
        == jnp.arange(n_experts * capacity, dtype=jnp.int32)[:, None, None]
    )
    dispatch = jnp.any(placement, axis=2).astype(jnp.bfloat16)
    outgoing = jnp.dot(dispatch, expert_in, preferred_element_type=jnp.float32).astype(jnp.bfloat16)
    outgoing = outgoing.reshape(n_experts, capacity, width)
    arrived = lax.all_to_all(outgoing, "ep", split_axis=0, concat_axis=0, tiled=True)
    sources, held, _ = arrived.shape
    flat = arrived.reshape(sources * held, width)
    hidden = expert_hidden(
        lax.all_gather(flat, "tp", axis=0, tiled=True), gate_weight[0], up_weight[0]
    )
    rows = hidden
    summed = lax.psum_scatter(
        jnp.dot(rows, down_weight[0], preferred_element_type=jnp.float32).astype(jnp.bfloat16),
        "tp",
        scatter_dimension=0,
        tiled=True,
    ).astype(jnp.float32)
    expert_out = lax.all_to_all(
        summed.reshape(sources, held, width).astype(jnp.bfloat16),
        "ep",
        split_axis=0,
        concat_axis=0,
        tiled=True,
    ).astype(jnp.float32)
    flat_out = expert_out.reshape(n_experts * capacity, width)
    picked = jnp.take(flat_out, targets, axis=0).reshape(rows_here, top_k, width)
    expert_mix = jnp.sum(picked * shares[:, :, None], axis=1).astype(jnp.bfloat16)
    return (mixed_tokens, expert_mix)


def solution(mesh):
    placed = (
        P(("grp", "ep", "tp"), None),
        P(),
        P(None, "tp"),
        P("tp", None, None),
        P("tp"),
        P("tp", None),
        P(("grp", "ep", "tp"), None),
        P(),
        P(("grp", "ep", "tp"), None),
        P(("grp", "ep", "tp"), None),
        P("ep", None, "tp"),
        P("ep", None, "tp"),
        P("ep", "tp", None),
    )
    return jax.shard_map(
        local,
        mesh=mesh,
        in_specs=placed,
        out_specs=(P(("grp", "ep", "tp"), None), P(("grp", "ep", "tp"), None)),
        check_vma=False,
    )
```
